512 devices in a mesh: ep: 128 (over z, x, core), tp: 4 (over y).
Axes of the slice: x: 4, y: 4, z: 16, core: 2. Of those that a mesh axis runs over, the one named last changes fastest.
Arguments:
- tokens: bfloat16 [16384, 2048], P('ep'), may hold values from -6 to 6
- pre_gain: float32 [2048], replicated, may hold values from 0.1 to 1.9
- post_gain: float32 [2048], P('tp'), may hold values from 0.1 to 1.9
- expert_ids: int32 [16384, 2], P('ep'), may hold values from 0 to 127, all different within a row; in each aligned block of 128 rows (0 to 127, 128 to 255, ...) at most 3 rows name the same one
- route_weights: float32 [16384, 2], P('ep'), may hold values from 0.1 to 1
- w_gate: bfloat16 [128, 2048, 512], P('ep', None, 'tp'), may hold values from -0.125 to 0.125
- w_up: bfloat16 [128, 2048, 512], P('ep', None, 'tp'), may hold values from -0.125 to 0.125
- w_down: bfloat16 [128, 512, 2048], P('ep', None, 'tp'), may hold values from -0.25 to 0.25
Outputs:
- routed: bfloat16 [16384, 2048], P('ep', 'tp')
The draws below stay inside these ranges and needn't reach their ends.
Inputs may be any that keep to these rules, and one draw needn't show every extreme that they name: `expert_ids`: each row names 2 different experts. Among the rows of one index of ep (aligned blocks of 128 rows) no expert is named by more than 3 rows, a bound that some block reaches.
All inputs are finite; a program needn't handle non-finite values.
Results may differ from the reference program's by a relative error of at most 0.007.
Values may be sent and summed in bfloat16 or wider, within the bound.
A program may use at most 64 MiB of HBM per device.

```python
import math
import jax
import jax.numpy as jnp
import numpy as np
from jax import lax

D = 2048
FF = 512
TOP = 2
TOK_EP = 128
EXPERTS = 128
CAP = 3
TOKENS = 16384
N_EP = 128


def levels(own_key, shape, shards, least, high):
    def one(dim, blocks):
        draws = jax.random.uniform(jax.random.fold_in(jax.random.fold_in(own_key, 6), dim), (blocks,), jnp.float32, least / len(shards), high / len(shards))
        return jnp.repeat(jnp.exp(draws), shape[dim] // blocks).reshape((-1,) + (1,) * (len(shape) - dim - 1))

    loudness = one(*shards[0])
    for cut in shards[1:]:
        loudness = loudness * one(*cut)
    return loudness


def routed_block(rng, own, number, rows, count, top, limit, slope):
    order = jax.random.permutation(rng, count)
    heavy_load, ordinary = portions_of(count, rows * top, limit, slope, True), portions_of(count, rows * top, limit, slope, False)
    places = jnp.arange(count)

    def named(tallies, offset_by):
        used = int((tallies > 0).sum())
        fixed = max(1, used // 4)
        shifted = fixed + (places - fixed + offset_by * (used - fixed)) % max(1, count - fixed)
        return jnp.zeros((count,), jnp.int32).at[order[jnp.where(places < fixed, places, shifted)]].set(jnp.asarray(tallies, jnp.int32))

    tallies = jnp.where(number % 4 == 0, named(heavy_load, number // 4), named(ordinary, number - number // 4 - 1))
    mixed = jax.random.permutation(jax.random.fold_in(own, 3), count)
    giver, receiver = mixed[0:count // 2 * 2:2], mixed[1:count // 2 * 2:2]
    room = jnp.minimum(tallies[giver] - 1, limit - tallies[receiver]) // 2
    room = jnp.where((giver == order[0]) | (receiver == order[0]) | (tallies[receiver] == 0), 0, jnp.maximum(room, 0))
    shifted = jax.random.randint(jax.random.fold_in(own, 4), (count // 2,), 0, 1 << 20) % (room + 1)
    tallies = tallies.at[giver].add(-shifted).at[receiver].add(shifted)
    labels = jnp.searchsorted(jnp.cumsum(tallies), jnp.arange(rows * top), side="right").astype(jnp.int32)
    table = labels.reshape(top, rows).T
    table = table[jax.random.permutation(jax.random.fold_in(own, 1), rows)]
    offset_by = jax.random.randint(jax.random.fold_in(own, 2), (rows, 1), 0, top)
    return jnp.take_along_axis(table, (jnp.arange(top)[None, :] + offset_by) % top, axis=1)


def portions_of(amount, total, reach, lean, full):
    loads = [(1 << 20) // math.isqrt(standing ** lean) + 1 for standing in range(1, amount + 1)]
    largest = reach if full else min(reach, max(-(-total // amount), total * loads[0] // sum(loads)))
    least = 1 if total - largest >= amount - 1 else 0
    counts, spare = [largest] + [least] * (amount - 1), total - largest - least * (amount - 1)
    while spare > 0:
        movable = [i for i in range(1, amount) if counts[i] < largest] or [i for i in range(1, amount) if counts[i] < reach]
        mass, left = sum([loads[i] for i in movable]), spare
        for i in movable:
            more = min(reach - counts[i], max(1, left * loads[i] // mass), spare)
            counts[i] = counts[i] + more
            spare = spare - more
    return np.array(counts)


def centred(key, dims, spread, bound, cuts=(), kind=jnp.bfloat16):
    loudness = levels(key, dims, cuts, -0.22, 0.18) if cuts else 1.0
    drawn = jax.random.normal(key, dims, jnp.float32) * spread * loudness
    return jnp.minimum(jnp.maximum(drawn, -bound), bound).astype(kind)


def setup_inputs(seed: int = 0) -> dict:
    key_of = jax.random.split(jax.random.key(seed), 9)
    tokens = centred(key_of[0], (TOKENS, D), 1.0, 6.0, ((0, 128),))
    pre_gain = jnp.clip(1.0 + 0.18 * jax.random.normal(key_of[1], (D,), jnp.float32), 0.1, 1.9)
    post_gain = jnp.clip(1.0 + 0.18 * jax.random.normal(key_of[2], (D,), jnp.float32), 0.1, 1.9)
    expert_ids_keys = jax.random.split(jax.random.fold_in(key_of[3], 1), TOKENS // TOK_EP)
    expert_ids_turns = jax.random.permutation(jax.random.fold_in(key_of[3], 3), TOKENS // TOK_EP)
    expert_ids = jax.vmap(lambda own, number: routed_block(jax.random.fold_in(key_of[3], 2), own, number, TOK_EP, EXPERTS, TOP, CAP, 2))(expert_ids_keys, expert_ids_turns).reshape((TOKENS, TOP))
    route_weights = jnp.clip(0.1 + 0.9 * jax.random.uniform(key_of[4], (TOKENS, TOP), jnp.float32) ** levels(key_of[4], (TOKENS, TOP), ((0, 128),), -0.2, 0.2), 0.1, 1.0)
    w_gate = centred(key_of[5], (EXPERTS, D, FF), D ** -0.5, 0.125, ((0, 128), (2, 4)))
    w_up = centred(key_of[6], (EXPERTS, D, FF), D ** -0.5, 0.125, ((0, 128), (2, 4)))
    w_down = centred(key_of[7], (EXPERTS, FF, D), FF ** -0.5, 0.25, ((0, 128), (2, 4)))
    return dict(tokens=tokens, pre_gain=pre_gain, post_gain=post_gain, expert_ids=expert_ids, route_weights=route_weights, w_gate=w_gate, w_up=w_up, w_down=w_down)


epsilon = 1e-06

def reference(tokens, pre_gain, post_gain, expert_ids, route_weights, w_gate, w_up, w_down):
    total_rows, row_width = tokens.shape
    values = tokens.astype(jnp.float32)
    row_scale = lax.rsqrt(lax.optimization_barrier(jnp.mean(values * values, axis=1, keepdims=True)) + epsilon)
    normed = (values * row_scale * pre_gain[None, :]).astype(jnp.bfloat16)
    expert_count = w_gate.shape[0]
    pick_count = expert_ids.shape[1]
    block_count = N_EP
    block_rows = total_rows // block_count
    pick_total = block_rows * pick_count
    flat_ids = expert_ids.reshape(block_count, pick_total).astype(jnp.int32)
    onehot = (flat_ids[:, :, None] == jnp.arange(expert_count, dtype=jnp.int32)[None, None, :]).astype(jnp.int32)
    earlier = jnp.cumsum(onehot, axis=1) - onehot
    slot_index = lax.optimization_barrier(jnp.sum(earlier * onehot, axis=2)).astype(jnp.int32)
    block_index = jnp.broadcast_to(jnp.arange(block_count, dtype=jnp.int32)[:, None], (block_count, pick_total))
    token_index = block_index * block_rows + (jnp.arange(pick_total, dtype=jnp.int32) // pick_count)[None, :]
    owners = jnp.full((expert_count, block_count, CAP), -1, jnp.int32).at[flat_ids, block_index, slot_index].set(token_index)
    weight_of = jnp.zeros((expert_count, block_count, CAP), jnp.float32).at[flat_ids, block_index, slot_index].set(route_weights.reshape(block_count, pick_total))

    def one_expert(mixed, items):
        owner_rows, weights, gate_w, up_w, down_w = items
        owner_rows = owner_rows.reshape(-1)
        live = owner_rows >= 0
        safe_rows = jnp.where(live, owner_rows, 0)
        gathered = normed[safe_rows]
        gate_sum = jnp.dot(gathered, gate_w, preferred_element_type=jnp.float32)
        up_sum = jnp.dot(gathered, up_w, preferred_element_type=jnp.float32)
        hidden = (jax.nn.silu(gate_sum) * up_sum).astype(jnp.bfloat16)
        expert_out = jnp.dot(hidden, down_w, preferred_element_type=jnp.float32).astype(jnp.bfloat16)
        expert_out = lax.optimization_barrier(expert_out).astype(jnp.float32)
        added = jnp.where(live[:, None], expert_out * weights.reshape(-1)[:, None], 0.0)
        return (mixed.at[safe_rows].add(added), None)
    start = jnp.zeros((total_rows, row_width), jnp.float32)
    mixed, _ = lax.scan(one_expert, start, (owners, weight_of, w_gate, w_up, w_down))
    out_scale = lax.rsqrt(lax.optimization_barrier(jnp.mean(mixed * mixed, axis=1, keepdims=True)) + epsilon)
    return (mixed * out_scale * post_gain[None, :]).astype(jnp.bfloat16)
```

```python
import jax
import jax.numpy as jnp
from jax import lax
from jax.experimental import pallas as pl
from jax.experimental.pallas import tpu as pltpu
from jax.sharding import PartitionSpec as P

epsilon = 1e-06
MESH = pl.DeviceIdType.MESH
NZ, NX, NC = 16, 4, 2
STEPS = (8, -7, 7, -6, 6, -5, 5, -4, 4, -3, 3, -2, 2, -1, 1, 0)
CHUNKS = 8


def places():
    me = lax.axis_index("ep")
    z, x, c = lax.div(me, NX * NC), lax.rem(lax.div(me, NC), NX), lax.rem(me, NC)
    return (
        [lax.rem(z + d, NZ) * (NX * NC) for d in range(NZ)],
        [lax.rem(x + d, NX) * NC for d in range(NX)],
        [c, 1 - c],
    )


def exchange_kernel(rows, x_ref, o_ref, send_sem, recv_sem):
    zs, xs, cs = places()

    def index(dz, q):
        return zs[dz % NZ] + xs[q // NC] + cs[q % NC]

    def back(dz, q):
        return zs[-dz % NZ] + xs[-(q // NC) % NX] + cs[q % NC]

    barrier = pltpu.get_barrier_semaphore()
    for dz in STEPS:
        for q in range(NX * NC):
            if dz or q:
                pl.semaphore_signal(barrier, inc=1, device_id={"ep": index(dz, q)}, device_id_type=MESH)
    pl.semaphore_wait(barrier, NZ * NX * NC - 1)
    for n, dz in enumerate(STEPS):
        for q in range(NX * NC):
            if not (dz or q):
                continue
            pltpu.make_async_remote_copy(
                x_ref.at[pl.ds(index(dz, q) * rows, rows)],
                o_ref.at[pl.ds((n * 8 + q) * rows, rows)],
                send_sem.at[n // 2],
                recv_sem.at[n // 2],
                device_id={"ep": index(dz, q)},
                device_id_type=MESH,
            ).start()
    own = (NZ * NX * NC - 8) * rows
    o_ref[own : own + rows] = x_ref[pl.ds(index(0, 0) * rows, rows)]
    for j in range(CHUNKS):
        pieces = [(j * 16 * rows, 16 * rows)] if j < 7 else [(112 * rows, 8 * rows), (121 * rows, 7 * rows)]
        total = sum(p[1] for p in pieces)
        part = o_ref.at[pl.ds(0, total)]
        pltpu.make_async_copy(part, part, send_sem.at[j]).wait()
        pltpu.make_async_copy(part, part, recv_sem.at[j]).wait()


def exchange(pieces, number):
    rows = pieces.shape[0] // 128
    return pl.pallas_call(
        lambda *refs: exchange_kernel(rows, *refs),
        out_shape=jax.ShapeDtypeStruct(pieces.shape, pieces.dtype),
        in_specs=[pl.BlockSpec(memory_space=pltpu.VMEM)],
        out_specs=pl.BlockSpec(memory_space=pltpu.VMEM),
        scratch_shapes=[pltpu.SemaphoreType.DMA((CHUNKS,)), pltpu.SemaphoreType.DMA((CHUNKS,))],
        compiler_params=pltpu.CompilerParams(collective_id=number, has_side_effects=True),
    )(pieces)


def joined_along(pieces, dim):
    shape = list(pieces.shape[1:])
    shape[dim] *= pieces.shape[0]
    return jnp.moveaxis(pieces, 0, dim).reshape(shape)


def gathered_copies(shard, axis, dim):
    length = lax.axis_size(axis)
    out = lax.all_to_all(jnp.broadcast_to(shard[None], (length, *shard.shape)), axis, 0, 0, tiled=True)
    return joined_along(out, dim)


def per_device(tokens, pre_gain, post_gain, expert_ids, route_weights, w_gate, w_up, w_down):
    tok_rows, row_width = tokens.shape
    pick_count = expert_ids.shape[1]
    experts = lax.axis_size("ep")
    capacity = 3
    pick_total = tok_rows * pick_count
    flat_ids = expert_ids.reshape(pick_total)
    onehot = (flat_ids[:, None] == jnp.arange(experts, dtype=jnp.int32)[None, :]).astype(jnp.bfloat16)
    positions = jnp.arange(pick_total, dtype=jnp.int32)
    strict_lower = (positions[None, :] < positions[:, None]).astype(jnp.bfloat16)
    earlier = jnp.dot(strict_lower, onehot, preferred_element_type=jnp.float32)
    slot_index = jnp.sum(earlier * onehot, axis=1).astype(jnp.int32)
    target = flat_ids * capacity + slot_index
    values = tokens.astype(jnp.float32)
    row_scale = lax.rsqrt(jnp.mean(values * values, axis=1, keepdims=True) + epsilon)
    normed = (values * row_scale * pre_gain[None, :]).astype(jnp.bfloat16)
    part_width = row_width // lax.axis_size("tp")
    outgoing = lax.dynamic_slice_in_dim(normed, lax.axis_index("tp") * part_width, part_width, 1)
    slots = jnp.arange(experts * capacity, dtype=jnp.int32)
    match = (target.reshape(1, tok_rows, pick_count) == slots[:, None, None])
    pick = match.any(axis=2).astype(jnp.bfloat16)
    buffer = jnp.dot(pick, outgoing)
    arrived = exchange(buffer.reshape(-1, 4, 128), 0).reshape(experts * capacity, part_width)
    block = gathered_copies(arrived, "tp", 1)
    gate_add = jnp.dot(block, w_gate[0], preferred_element_type=jnp.float32)
    up_add = jnp.dot(block, w_up[0], preferred_element_type=jnp.float32)
    hidden = (jax.nn.silu(gate_add) * up_add).astype(jnp.bfloat16)
    piece = gathered_copies(hidden, "tp", 1)
    produced = jnp.dot(piece, w_down[0], preferred_element_type=jnp.float32).astype(jnp.bfloat16)
    me = lax.axis_index("ep")
    z, x, c = me // 8, (me // 2) % 4, me % 2
    steps = jnp.array(STEPS, jnp.int32)
    spot = jnp.zeros((NZ,), jnp.int32).at[steps % NZ].set(jnp.arange(NZ, dtype=jnp.int32))
    other = jnp.arange(experts, dtype=jnp.int32)
    zo, xo, co = other // 8, (other // 2) % 4, other % 2
    place = spot[(z - zo) % NZ] * 8 + ((x - xo) % 4) * 2 + (c - co) % 2
    by_device = produced.reshape(experts, capacity, -1)[place].reshape(-1, 4, 128)
    came = exchange(by_device, 1).reshape(experts, capacity, -1)
    home = spot[(z - zo) % NZ] * 8 + ((x - xo) % 4) * 2 + (c - co) % 2
    returned = came[home].reshape(experts * capacity, -1)
    picked = returned[target].astype(jnp.float32) * route_weights.reshape(pick_total)[:, None]
    mixed = jnp.sum(picked.reshape(tok_rows, pick_count, -1), axis=1)
    squares = lax.all_gather(jnp.sum(mixed * mixed, axis=1), "tp").sum(axis=0)
    out_scale = lax.rsqrt(squares / row_width + epsilon)
    return (mixed * out_scale[:, None] * post_gain[None, :]).astype(jnp.bfloat16)


def solution(mesh):
    in_specs = (
        P("ep", None),
        P(),
        P("tp"),
        P("ep", None),
        P("ep", None),
        P("ep", None, "tp"),
        P("ep", None, "tp"),
        P("ep", None, "tp"),
    )
    return jax.shard_map(per_device, mesh=mesh, in_specs=in_specs, out_specs=P("ep", "tp"), check_vma=False)
```

```python
import jax
import jax.numpy as jnp
from jax import lax
from jax.experimental import pallas as pl
from jax.experimental.pallas import tpu as pltpu
from jax.sharding import PartitionSpec as P

epsilon = 1e-06
MESH = pl.DeviceIdType.MESH
NZ, NX, NC, NY = 16, 4, 2, 4
NQ = NX * NC
PEERS = NZ * NQ
CAP = 3
STEPS = (8, -7, 7, -6, 6, -5, 5, -4, 4, -3, 3, -2, 2, -1, 1, 0)
CHUNKS = 8
PER = PEERS // CHUNKS
ROWS = PER * CAP
LANES = 128
PARTS = 4
BLOCK = PARTS * CAP
TALL = PER * BLOCK
BF16, F32, I32 = jnp.bfloat16, jnp.float32, jnp.int32


def dot(a, b):
    return jnp.dot(a, b, preferred_element_type=F32)


def iota(shape, dim):
    return lax.broadcasted_iota(I32, shape, dim)


def tall_row(wide):
    part = sum((wide >= ROWS * k).astype(I32) for k in range(1, PARTS))
    rest = wide - part * ROWS
    block = (rest * 171) >> 9
    return block * BLOCK + part * CAP + (rest - block * CAP)


def kernel(
    tokens_hbm, pre_ref, post_ref, ids_ref, weights_ref, gate_hbm, up_hbm, down_hbm,
    o_ref,
    tokens, gate_up, down, sent, arrived, gathered, hidden, results, returned, squares,
    load_sem, out_sem, in_sem, feat_out, feat_in, hid_out, hid_in, ret_out, ret_in, sq_sem,
):
    me, y = lax.axis_index("ep"), lax.axis_index("tp")
    z, x, c = lax.div(me, NQ), lax.rem(lax.div(me, NC), NX), lax.rem(me, NC)
    zs = [lax.rem(z + d, NZ) * NQ for d in range(NZ)]
    xs = [lax.rem(x + d, NX) * NC for d in range(NX)]
    cs = [c, 1 - c]
    ys = [lax.rem(y + d, NY) for d in (1, 3, 2)]

    def ahead(n, q):
        return {"ep": zs[STEPS[n] % NZ] + xs[q // NC] + cs[q % NC]}

    def behind(n, q):
        return {"ep": zs[-STEPS[n] % NZ] + xs[-(q // NC) % NX] + cs[q % NC]}

    barrier = pltpu.get_barrier_semaphore()
    for n in range(NZ):
        for q in range(NQ):
            if STEPS[n] or q:
                pl.semaphore_signal(barrier, inc=1, device_id=ahead(n, q), device_id_type=MESH)
    for other in ys:
        pl.semaphore_signal(barrier, inc=1, device_id={"tp": other}, device_id_type=MESH)

    loads = [
        pltpu.make_async_copy(tokens_hbm, tokens, load_sem.at[0]),
        pltpu.make_async_copy(gate_hbm.at[0], gate_up.at[:, pl.ds(0, LANES)], load_sem.at[1]),
        pltpu.make_async_copy(up_hbm.at[0], gate_up.at[:, pl.ds(LANES, LANES)], load_sem.at[2]),
        pltpu.make_async_copy(down_hbm.at[0], down, load_sem.at[3]),
    ]
    for load in loads:
        load.start()

    rows = tokens.shape[0]
    lane = iota((rows, PEERS), 1)
    lower = (iota((rows, rows), 1) < iota((rows, rows), 0)).astype(BF16)
    spots, before = [], None
    for k in range(2):
        e = ids_ref[:, k : k + 1]
        dz = ((e >> 3) - z) & (NZ - 1)
        n = sum(jnp.where(dz == STEPS[i] % NZ, i, 0) for i in range(NZ))
        q = (((((e >> 1) & 3) - x) & 3) << 1) + (((e & 1) - c) & 1)
        p = n * NQ + q
        mark = (lane == p).astype(F32)
        earlier = dot(lower, mark.astype(BF16))
        if before is not None:
            earlier = earlier + before
        before = jnp.sum(mark, axis=0, keepdims=True)
        slot = jnp.sum(earlier * mark, axis=1, keepdims=True)
        spots.append(p * BLOCK + slot.astype(I32))
    across = []
    for spot in spots:
        row = jnp.transpose(jnp.broadcast_to(spot.astype(F32), (rows, rows)))[0:1, :].astype(I32)
        across.append(jnp.concatenate([row + CAP * part for part in range(PARTS)], axis=1))

    loads[0].wait()
    values = tokens[...].astype(F32)
    scale = lax.rsqrt(jnp.mean(values * values, axis=1, keepdims=True) + epsilon)
    width = PARTS * LANES
    mine = pl.ds(pl.multiple_of(y * width, width), width)
    normed = (tokens[:, mine].astype(F32) * scale * pre_ref[:, mine]).astype(BF16)
    stacked = jnp.concatenate([normed[:, part * LANES : (part + 1) * LANES] for part in range(PARTS)], axis=0)

    flat_sent = sent.reshape(PEERS * BLOCK, LANES)
    flat_arrived = arrived.reshape(PEERS * BLOCK, LANES)
    flat_results = results.reshape(PEERS * BLOCK, LANES)
    flat_returned = returned.reshape(PEERS * BLOCK, LANES)
    for j in range(CHUNKS):
        r = iota((TALL, rows * PARTS), 0) + j * TALL
        take = jnp.where((r == across[0]) | (r == across[1]), 1.0, 0.0).astype(BF16)
        flat_sent[j * TALL : (j + 1) * TALL, :] = dot(take, stacked).astype(BF16)

    own = (PEERS - NQ) * CAP
    pl.semaphore_wait(barrier, PEERS - 1 + NY - 1)

    def send_blocks(source, target, sends, receives, j, place):
        for b in range(PER):
            n, q = divmod(j * PER + b, NQ)
            if not (STEPS[n] or q):
                continue
            at = pl.ds((j * PER + b) * CAP, CAP)
            pltpu.make_async_remote_copy(
                source.at[at], target.at[at], sends.at[j], receives.at[j], device_id=place(n, q), device_id_type=MESH
            ).start()

    def wait_blocks(buffer, sem, j):
        count = ROWS if j < CHUNKS - 1 else ROWS - CAP
        part = buffer.at[pl.ds(0, count)]
        pltpu.make_async_copy(part, part, sem.at[j]).wait()

    def send_tp(buffer, sends, receives, j):
        for other in ys:
            pltpu.make_async_remote_copy(
                buffer.at[j, y], buffer.at[j, y], sends.at[j], receives.at[j],
                device_id={"tp": other}, device_id_type=MESH,
            ).start()

    def wait_tp(buffer, sem, j):
        part = buffer.at[j, pl.ds(0, NY - 1)]
        pltpu.make_async_copy(part, part, sem.at[j]).wait()

    for j in range(CHUNKS):
        send_blocks(sent, arrived, out_sem, in_sem, j, ahead)
    arrived[own : own + CAP] = sent[own : own + CAP]

    to_wide = (iota((TALL, TALL), 1) == tall_row(iota((TALL, TALL), 0))).astype(BF16)
    to_tall = (iota((TALL, TALL), 0) == tall_row(iota((TALL, TALL), 1))).astype(BF16)

    def collect(j):
        wait_blocks(arrived, in_sem, j)
        wide = dot(to_wide, flat_arrived[j * TALL : (j + 1) * TALL, :]).astype(BF16)
        wide = jnp.concatenate([wide[part * ROWS : (part + 1) * ROWS] for part in range(PARTS)], axis=1)
        gathered[j, y] = wide
        send_tp(gathered, feat_out, feat_in, j)

    def gated(j):
        wait_tp(gathered, feat_in, j)
        total = sum(dot(gathered[j, other], gate_up[other * width : (other + 1) * width, :]) for other in range(NY))
        gate, up = total[:, :LANES], total[:, LANES:]
        hidden[j, y] = (gate / (1.0 + jnp.exp(-gate)) * up).astype(BF16)
        send_tp(hidden, hid_out, hid_in, j)

    def project(j):
        wait_tp(hidden, hid_in, j)
        units = jnp.concatenate([hidden[j, other] for other in range(NY)], axis=1)
        made = dot(units, down[...]).astype(BF16)
        made = jnp.concatenate([made[:, part * LANES : (part + 1) * LANES] for part in range(PARTS)], axis=0)
        flat_results[j * TALL : (j + 1) * TALL, :] = dot(to_tall, made).astype(BF16)
        send_blocks(results, returned, ret_out, ret_in, j, behind)
        if j == CHUNKS - 1:
            returned[own : own + CAP] = results[own : own + CAP]

    for load in loads[1:]:
        load.wait()
    for step in range(CHUNKS + 2):
        if step < CHUNKS:
            collect(step)
        if 0 <= step - 1 < CHUNKS:
            gated(step - 1)
        if 0 <= step - 2 < CHUNKS:
            project(step - 2)

    mixed = jnp.zeros((rows * PARTS, LANES), F32)
    for j in range(CHUNKS):
        r = iota((rows, TALL), 1) + j * TALL
        share = jnp.concatenate(
            [
                sum(jnp.where(r == spots[k] + CAP * part, weights_ref[:, k : k + 1], 0.0) for k in range(2))
                for part in range(PARTS)
            ],
            axis=0,
        )
        coarse = share.astype(BF16)
        fine = (share - coarse.astype(F32)).astype(BF16)
        wait_blocks(returned, ret_in, j)
        back = flat_returned[j * TALL : (j + 1) * TALL, :]
        mixed = mixed + (dot(coarse, back) + dot(fine, back))
    pieces = [mixed[part * rows : (part + 1) * rows] for part in range(PARTS)]

    square = jnp.sum(sum(piece * piece for piece in pieces), axis=1, keepdims=True)
    squares[y] = jnp.transpose(jnp.broadcast_to(square, (rows, rows)))[0:1, :]
    for other in ys:
        pltpu.make_async_remote_copy(
            squares.at[y], squares.at[y], sq_sem.at[0], sq_sem.at[1], device_id={"tp": other}, device_id_type=MESH
        ).start()
    for j in range(CHUNKS):
        wait_blocks(sent, out_sem, j)
        wait_blocks(results, ret_out, j)
        wait_tp(gathered, feat_out, j)
        wait_tp(hidden, hid_out, j)
    three = squares.at[pl.ds(0, NY - 1)]
    pltpu.make_async_copy(three, three, sq_sem.at[1]).wait()
    total = squares[0] + squares[1] + squares[2] + squares[3]
    total = jnp.transpose(jnp.broadcast_to(total, (rows, rows)))
    out_scale = lax.rsqrt(total / (width * NY) + epsilon)
    for part in range(PARTS):
        at = slice(part * LANES, (part + 1) * LANES)
        o_ref[:, at] = (pieces[part] * out_scale * post_ref[:, at]).astype(BF16)
    pltpu.make_async_copy(three, three, sq_sem.at[0]).wait()


def per_device(tokens, pre_gain, post_gain, expert_ids, route_weights, w_gate, w_up, w_down):
    rows, row_width = tokens.shape
    width = PARTS * LANES
    blocks = pltpu.VMEM((PEERS * CAP, PARTS, LANES), BF16)
    sems = pltpu.SemaphoreType.DMA((CHUNKS,))
    vmem, hbm = pl.BlockSpec(memory_space=pltpu.VMEM), pl.BlockSpec(memory_space=pl.ANY)
    return pl.pallas_call(
        kernel,
        out_shape=jax.ShapeDtypeStruct((rows, width), BF16),
        in_specs=[hbm, vmem, vmem, vmem, vmem, hbm, hbm, hbm],
        out_specs=vmem,
        scratch_shapes=[
            pltpu.VMEM((rows, row_width), BF16),
            pltpu.VMEM((row_width, 2 * LANES), BF16),
            pltpu.VMEM((w_down.shape[1], width), BF16),
            blocks,
            blocks,
            pltpu.VMEM((CHUNKS, NY, ROWS, width), BF16),
            pltpu.VMEM((CHUNKS, NY, ROWS, LANES), BF16),
            blocks,
            blocks,
            pltpu.VMEM((NY, 1, rows), F32),
            pltpu.SemaphoreType.DMA((4,)),
            *[sems] * 8,
            pltpu.SemaphoreType.DMA((2,)),
        ],
        compiler_params=pltpu.CompilerParams(collective_id=0, has_side_effects=True),
    )(tokens, pre_gain[None, :], post_gain[None, :], expert_ids, route_weights, w_gate, w_up, w_down)


def solution(mesh):
    in_specs = (
        P("ep", None),
        P(),
        P("tp"),
        P("ep", None),
        P("ep", None),
        P("ep", None, "tp"),
        P("ep", None, "tp"),
        P("ep", None, "tp"),
    )
    return jax.shard_map(per_device, mesh=mesh, in_specs=in_specs, out_specs=P("ep", "tp"), check_vma=False)
```

```python
import jax
import jax.numpy as jnp
from jax import lax
from jax.experimental import pallas as pl
from jax.experimental.pallas import tpu as pltpu
from jax.sharding import PartitionSpec as P

epsilon = 1e-06
MESH = pl.DeviceIdType.MESH
NZ, NX, NC, NY = 16, 4, 2, 4
NQ = NX * NC
PEERS = NZ * NQ
CAP = 3
STEPS = (0, 1, -1, 2, -2, 3, -3, 4, 8, -7, 7, -6, 6, -5, 5, -4)
PLAN = (
    "K0", "S0", "S1", "K1", "S2", "S3", "K2", "S4", "S5", "S6", "S7", "C0", "C1", "C2", "C3", "G0", "G1", "G2",
    "G3", "P0", "C4", "P1", "P2", "P3", "C5", "G4", "C6", "G5", "P4", "C7", "G6", "P5", "G7", "P6", "P7", "M0",
    "M1", "M2", "M3", "M4", "M5", "M6", "M7",
)
NEAR = 2
CHUNKS = 8
PER = PEERS // CHUNKS
ROWS = PER * CAP
LANES = 128
PARTS = 4
BLOCK = PARTS * CAP
TALL = PER * BLOCK
BF16, F32, I32 = jnp.bfloat16, jnp.float32, jnp.int32


def dot(a, b):
    return jnp.dot(a, b, preferred_element_type=F32)


def iota(shape, dim):
    return lax.broadcasted_iota(I32, shape, dim)


def tall_row(wide):
    part = sum((wide >= ROWS * k).astype(I32) for k in range(1, PARTS))
    rest = wide - part * ROWS
    block = (rest * 171) >> 9
    return block * BLOCK + part * CAP + (rest - block * CAP)


def kernel(
    tokens_hbm, pre_hbm, ids_hbm, weights_hbm, gate_hbm, up_hbm, down_hbm,
    o_ref,
    tokens, pre, ids, weights, gate_up, down, sent, arrived, gathered, hidden, results, returned, squares, mixed,
    load_sem, wide_sem, out_sem, in_sem, feat_out, feat_in, hid_out, hid_in, ret_out, ret_in, sq_sem,
):
    me, y = lax.axis_index("ep"), lax.axis_index("tp")
    z, x, c = lax.div(me, NQ), lax.rem(lax.div(me, NC), NX), lax.rem(me, NC)
    zs = [lax.rem(z + d, NZ) * NQ for d in range(NZ)]
    xs = [lax.rem(x + d, NX) * NC for d in range(NX)]
    cs = [c, 1 - c]
    ys = [lax.rem(y + d, NY) for d in (1, 3, 2)]

    def at(dz, q):
        return {"ep": zs[dz % NZ] + xs[q // NC] + cs[q % NC]}

    def ahead(n, q):
        return at(STEPS[n], q)

    def behind(n, q):
        return {"ep": zs[-STEPS[n] % NZ] + xs[-(q // NC) % NX] + cs[q % NC]}

    barrier = pltpu.get_barrier_semaphore()
    for other in ys:
        pl.semaphore_signal(barrier, inc=1, device_id={"tp": other}, device_id_type=MESH)
    for dz in range(-NEAR, NEAR + 1):
        for q in range(NQ):
            if dz or q:
                pl.semaphore_signal(barrier, inc=1, device_id=at(dz, q), device_id_type=MESH)

    def hear(level):
        if level == 0:
            pl.semaphore_wait(barrier, (2 * NEAR + 1) * NQ - 1 + NY - 1)
        else:
            pl.semaphore_wait(wide_sem.at[level - 1], 2)
        reach = NEAR << level
        if reach < NZ // 2:
            for dz in (reach, -reach):
                pl.semaphore_signal(wide_sem.at[level], inc=1, device_id=at(dz, 0), device_id_type=MESH)

    loads = [
        pltpu.make_async_copy(ids_hbm, ids, load_sem.at[0]),
        pltpu.make_async_copy(tokens_hbm, tokens, load_sem.at[1]),
        pltpu.make_async_copy(pre_hbm, pre, load_sem.at[2]),
        pltpu.make_async_copy(weights_hbm, weights, load_sem.at[3]),
        pltpu.make_async_copy(gate_hbm.at[0], gate_up.at[:, pl.ds(0, LANES)], load_sem.at[4]),
        pltpu.make_async_copy(up_hbm.at[0], gate_up.at[:, pl.ds(LANES, LANES)], load_sem.at[5]),
        pltpu.make_async_copy(down_hbm.at[0], down, load_sem.at[6]),
    ]
    for load in loads:
        load.start()

    rows = tokens.shape[0]
    square_shape = (rows, rows)
    earlier_than = (iota(square_shape, 0) < iota(square_shape, 1)).astype(BF16)
    loads[0].wait()
    spots, before = [], None
    for k in range(2):
        e = ids[k : k + 1, :]
        dz = ((e >> 3) - z) & (NZ - 1)
        n = sum(jnp.where(dz == STEPS[i] % NZ, i, 0) for i in range(NZ))
        q = (((((e >> 1) & 3) - x) & 3) << 1) + (((e & 1) - c) & 1)
        p = n * NQ + q
        mark = (iota((PEERS, rows), 0) == p).astype(F32)
        earlier = dot(mark.astype(BF16), earlier_than)
        if before is not None:
            earlier = earlier + before
        before = jnp.sum(mark, axis=1, keepdims=True)
        slot = jnp.sum(earlier * mark, axis=0, keepdims=True)
        spots.append(p * BLOCK + slot.astype(I32))
    across = [jnp.concatenate([spot + CAP * part for part in range(PARTS)], axis=1) for spot in spots]

    loads[1].wait()
    loads[2].wait()
    values = tokens[...].astype(F32)
    scale = lax.rsqrt(jnp.mean(values * values, axis=1, keepdims=True) + epsilon)
    width = PARTS * LANES
    mine = pl.ds(pl.multiple_of(y * width, width), width)
    normed = (tokens[:, mine].astype(F32) * scale * pre[:, mine]).astype(BF16)
    stacked = jnp.concatenate([normed[:, part * LANES : (part + 1) * LANES] for part in range(PARTS)], axis=0)

    flat_sent = sent.reshape(PEERS * BLOCK, LANES)
    flat_arrived = arrived.reshape(PEERS * BLOCK, LANES)
    flat_results = results.reshape(PEERS * BLOCK, LANES)
    flat_returned = returned.reshape(PEERS * BLOCK, LANES)
    own_chunk, own = STEPS.index(0) // 2, STEPS.index(0) * NQ * CAP

    def send_blocks(source, target, sends, receives, j, place):
        for b in range(PER):
            n, q = divmod(j * PER + b, NQ)
            if not (STEPS[n] or q):
                continue
            rows_at = pl.ds((j * PER + b) * CAP, CAP)
            pltpu.make_async_remote_copy(
                source.at[rows_at], target.at[rows_at], sends.at[j], receives.at[j],
                device_id=place(n, q), device_id_type=MESH,
            ).start()
        if j == own_chunk:
            target[own : own + CAP] = source[own : own + CAP]

    def wait_blocks(buffer, sem, j):
        part = buffer.at[pl.ds(0, ROWS - CAP if j == own_chunk else ROWS)]
        pltpu.make_async_copy(part, part, sem.at[j]).wait()

    def send_tp(buffer, sends, receives, j):
        for other in ys:
            pltpu.make_async_remote_copy(
                buffer.at[j, y], buffer.at[j, y], sends.at[j], receives.at[j],
                device_id={"tp": other}, device_id_type=MESH,
            ).start()

    def wait_tp(buffer, sem, j):
        part = buffer.at[j, pl.ds(0, NY - 1)]
        pltpu.make_async_copy(part, part, sem.at[j]).wait()

    def assemble(j):
        r = iota((TALL, rows * PARTS), 0) + j * TALL
        take = jnp.where((r == across[0]) | (r == across[1]), 1.0, 0.0).astype(BF16)
        flat_sent[j * TALL : (j + 1) * TALL, :] = dot(take, stacked).astype(BF16)

    def send(j):
        if j + 1 < CHUNKS:
            assemble(j + 1)
        send_blocks(sent, arrived, out_sem, in_sem, j, ahead)

    to_wide = (iota((TALL, TALL), 1) == tall_row(iota((TALL, TALL), 0))).astype(BF16)
    to_tall = (iota((TALL, TALL), 0) == tall_row(iota((TALL, TALL), 1))).astype(BF16)

    def collect(j):
        wait_blocks(arrived, in_sem, j)
        wide = dot(to_wide, flat_arrived[j * TALL : (j + 1) * TALL, :]).astype(BF16)
        wide = jnp.concatenate([wide[part * ROWS : (part + 1) * ROWS] for part in range(PARTS)], axis=1)
        gathered[j, y] = wide
        send_tp(gathered, feat_out, feat_in, j)

    def gated(j):
        if j == 0:
            for load in loads[3:]:
                load.wait()
        wait_tp(gathered, feat_in, j)
        total = sum(dot(gathered[j, other], gate_up[other * width : (other + 1) * width, :]) for other in range(NY))
        gate, up = total[:, :LANES], total[:, LANES:]
        hidden[j, y] = (gate / (1.0 + jnp.exp(-gate)) * up).astype(BF16)
        send_tp(hidden, hid_out, hid_in, j)

    def project(j):
        wait_tp(hidden, hid_in, j)
        units = jnp.concatenate([hidden[j, other] for other in range(NY)], axis=1)
        made = dot(units, down[...]).astype(BF16)
        made = jnp.concatenate([made[:, part * LANES : (part + 1) * LANES] for part in range(PARTS)], axis=0)
        flat_results[j * TALL : (j + 1) * TALL, :] = dot(to_tall, made).astype(BF16)
        send_blocks(results, returned, ret_out, ret_in, j, behind)

    def column(row):
        return jnp.transpose(jnp.broadcast_to(row, square_shape))[:, 0:1]

    columns = []

    def merge(j):
        if not columns:
            columns.extend((column(spots[k].astype(F32)).astype(I32), column(weights[k : k + 1, :])) for k in range(2))
        r = iota((rows, TALL), 1) + j * TALL
        share = jnp.concatenate(
            [sum(jnp.where(r == s + CAP * part, w, 0.0) for s, w in columns) for part in range(PARTS)], axis=0
        )
        coarse = share.astype(BF16)
        fine = (share - coarse.astype(F32)).astype(BF16)
        wait_blocks(returned, ret_in, j)
        back = flat_returned[j * TALL : (j + 1) * TALL, :]
        added = dot(coarse, back) + dot(fine, back)
        mixed[...] = added if j == 0 else mixed[...] + added

    assemble(0)
    steps = dict(K=hear, S=send, C=collect, G=gated, P=project, M=merge)
    for step in PLAN:
        steps[step[0]](int(step[1:]))

    pieces = [mixed[part * rows : (part + 1) * rows, :] for part in range(PARTS)]
    square = jnp.sum(sum(piece * piece for piece in pieces), axis=1, keepdims=True)
    squares[y] = jnp.transpose(jnp.broadcast_to(square, square_shape))[0:1, :]
    for other in ys:
        pltpu.make_async_remote_copy(
            squares.at[y], squares.at[y], sq_sem.at[0], sq_sem.at[1], device_id={"tp": other}, device_id_type=MESH
        ).start()
    for j in range(CHUNKS):
        wait_blocks(sent, out_sem, j)
        wait_blocks(results, ret_out, j)
        wait_tp(gathered, feat_out, j)
        wait_tp(hidden, hid_out, j)
    three = squares.at[pl.ds(0, NY - 1)]
    pltpu.make_async_copy(three, three, sq_sem.at[1]).wait()
    total = squares[0] + squares[1] + squares[2] + squares[3]
    out_scale = lax.rsqrt(total / (width * NY) + epsilon)
    out_scale = jnp.transpose(jnp.broadcast_to(out_scale, square_shape))
    for part in range(PARTS):
        o_ref[:, part * LANES : (part + 1) * LANES] = pieces[part] * out_scale
    pltpu.make_async_copy(three, three, sq_sem.at[0]).wait()


def per_device(tokens, pre_gain, post_gain, expert_ids, route_weights, w_gate, w_up, w_down):
    rows, row_width = tokens.shape
    width = PARTS * LANES
    blocks = pltpu.VMEM((PEERS * CAP, PARTS, LANES), BF16)
    sems = pltpu.SemaphoreType.DMA((CHUNKS,))
    scaled = pl.pallas_call(
        kernel,
        out_shape=pltpu.VMEM((rows, width), F32),
        in_specs=[pl.BlockSpec(memory_space=pltpu.HBM)] * 7,
        out_specs=pl.BlockSpec(memory_space=pltpu.VMEM),
        scratch_shapes=[
            pltpu.VMEM((rows, row_width), BF16),
            pltpu.VMEM((1, row_width), F32),
            pltpu.VMEM((2, rows), I32),
            pltpu.VMEM((2, rows), F32),
            pltpu.VMEM((row_width, 2 * LANES), BF16),
            pltpu.VMEM((w_down.shape[1], width), BF16),
            blocks,
            blocks,
            pltpu.VMEM((CHUNKS, NY, ROWS, width), BF16),
            pltpu.VMEM((CHUNKS, NY, ROWS, LANES), BF16),
            blocks,
            blocks,
            pltpu.VMEM((NY, 1, rows), F32),
            pltpu.VMEM((rows * PARTS, LANES), F32),
            pltpu.SemaphoreType.DMA((7,)),
            pltpu.SemaphoreType.REGULAR((3,)),
            *[sems] * 8,
            pltpu.SemaphoreType.DMA((2,)),
        ],
        compiler_params=pltpu.CompilerParams(
            collective_id=0, has_side_effects=True
        ),
    )(tokens, pre_gain[None, :], expert_ids.T, route_weights.T, w_gate, w_up, w_down)
    return (scaled * post_gain[None, :]).astype(BF16)


def solution(mesh):
    in_specs = (
        P("ep", None),
        P(),
        P("tp"),
        P("ep", None),
        P("ep", None),
        P("ep", None, "tp"),
        P("ep", None, "tp"),
        P("ep", None, "tp"),
    )
    return jax.shard_map(per_device, mesh=mesh, in_specs=in_specs, out_specs=P("ep", "tp"), check_vma=False)
```

```python
import jax
import jax.numpy as jnp
from jax import lax
from jax.experimental import pallas as pl
from jax.experimental.pallas import tpu as pltpu
from jax.sharding import PartitionSpec as P

epsilon = 1e-06
MESH = pl.DeviceIdType.MESH
NZ, NX, NC, NY = 16, 4, 2, 4
NQ = NX * NC
PEERS = NZ * NQ
FARTHEST = (5, 4, 3, 7, 2, 6, 1, 0)
CAP = 3
STEPS = (0, 1, -1, 2, -2, 3, 4, -4, -3, 8, -7, 7, -6, 6, -5, 5)
PLAN = (
    "A0", "A1", "A2", "A3", "K0", "S0", "S1", "A4", "A5", "K1", "S2", "S3", "A6", "A7", "K2", "S4", "S5", "S6",
    "S7", "C0", "C1", "C2", "C3", "G0", "G1", "G2", "G3", "P0", "C4", "P1", "P2", "C5", "P3", "G4", "C6", "G5",
    "P4", "C7", "G6", "P5", "G7", "P6", "P7", "M0", "M1", "M2", "M3", "M4", "M5", "M6", "M7",
)
NEAR = 2
EDGES = (0, 2, 4, 6, 8, 10, 12, 14, 16)
CHUNKS = len(EDGES) - 1
SPAN = [EDGES[j + 1] - EDGES[j] for j in range(CHUNKS)]
ROWS = [NQ * CAP * span for span in SPAN]
LANES = 128
PARTS = 4
BLOCK = PARTS * CAP
TALL = [NQ * BLOCK * span for span in SPAN]
BASE = [NQ * BLOCK * edge for edge in EDGES]
BF16, F32, I32 = jnp.bfloat16, jnp.float32, jnp.int32


def dot(a, b):
    return jnp.dot(a, b, preferred_element_type=F32)


def iota(shape, dim):
    return lax.broadcasted_iota(I32, shape, dim)


def tall_row(wide, rows):
    part = sum((wide >= rows * k).astype(I32) for k in range(1, PARTS))
    rest = wide - part * rows
    block = (rest * 171) >> 9
    return block * BLOCK + part * CAP + (rest - block * CAP)


def kernel(
    tokens_hbm, pre_hbm, ids_hbm, weights_hbm, gate_hbm, up_hbm, down_hbm,
    o_ref,
    tokens, pre, ids, weights, gate_up, down, sent, arrived, results, returned, squares, mixed,
    load_sem, wide_sem, out_sem, in_sem, feat_out, feat_in, hid_out, hid_in, ret_out, ret_in, sq_sem, *buffers,
):
    gathered, hidden = buffers[:CHUNKS], buffers[CHUNKS:]
    me, y = lax.axis_index("ep"), lax.axis_index("tp")
    z, x, c = lax.div(me, NQ), lax.rem(lax.div(me, NC), NX), lax.rem(me, NC)
    zs = [lax.rem(z + d, NZ) * NQ for d in range(NZ)]
    xs = [lax.rem(x + d, NX) * NC for d in range(NX)]
    cs = [c, 1 - c]
    ys = [lax.rem(y + d, NY) for d in (2, 1, 3)]

    def at(dz, q):
        return {"ep": zs[dz % NZ] + xs[q // NC] + cs[q % NC]}

    def ahead(n, q):
        return at(STEPS[n], q)

    def behind(n, q):
        return {"ep": zs[-STEPS[n] % NZ] + xs[-(q // NC) % NX] + cs[q % NC]}

    barrier = pltpu.get_barrier_semaphore()
    for other in ys:
        pl.semaphore_signal(barrier, inc=1, device_id={"tp": other}, device_id_type=MESH)
    near = range(max(-NEAR, 1 - NZ // 2), NEAR + 1)
    for dz in sorted(near, key=abs, reverse=True):
        for q in FARTHEST:
            if dz or q:
                pl.semaphore_signal(barrier, inc=1, device_id=at(dz, q), device_id_type=MESH)

    def hear(level):
        if level == 0:
            pl.semaphore_wait(barrier, len(near) * NQ - 1 + NY - 1)
        else:
            pl.semaphore_wait(wide_sem.at[level - 1], 2)
        reach = NEAR << level
        if reach < NZ // 2:
            for dz in (reach, -reach):
                pl.semaphore_signal(wide_sem.at[level], inc=1, device_id=at(dz, 0), device_id_type=MESH)

    loads = [
        pltpu.make_async_copy(ids_hbm, ids, load_sem.at[0]),
        pltpu.make_async_copy(tokens_hbm, tokens, load_sem.at[1]),
        pltpu.make_async_copy(pre_hbm, pre, load_sem.at[2]),
        pltpu.make_async_copy(weights_hbm, weights, load_sem.at[3]),
        pltpu.make_async_copy(gate_hbm.at[0], gate_up.at[:, pl.ds(0, LANES)], load_sem.at[4]),
        pltpu.make_async_copy(up_hbm.at[0], gate_up.at[:, pl.ds(LANES, LANES)], load_sem.at[5]),
        pltpu.make_async_copy(down_hbm.at[0], down, load_sem.at[6]),
    ]
    for load in loads:
        load.start()

    rows = tokens.shape[0]
    square_shape = (rows, rows)
    earlier_than = (iota(square_shape, 0) < iota(square_shape, 1)).astype(BF16)
    loads[0].wait()
    spots, before = [], None
    for k in range(2):
        e = ids[k : k + 1, :]
        dz = ((e >> 3) - z) & (NZ - 1)
        n = sum(jnp.where(dz == STEPS[i] % NZ, i, 0) for i in range(NZ))
        q = (((((e >> 1) & 3) - x) & 3) << 1) + (((e & 1) - c) & 1)
        p = n * NQ + q
        mark = (iota((PEERS, rows), 0) == p).astype(F32)
        earlier = dot(mark.astype(BF16), earlier_than)
        if before is not None:
            earlier = earlier + before
        before = jnp.sum(mark, axis=1, keepdims=True)
        slot = jnp.sum(earlier * mark, axis=0, keepdims=True)
        spots.append(p * BLOCK + slot.astype(I32))
    across = [jnp.concatenate([spot + CAP * part for part in range(PARTS)], axis=1) for spot in spots]

    loads[1].wait()
    loads[2].wait()
    values = tokens[...].astype(F32)
    scale = lax.rsqrt(jnp.mean(values * values, axis=1, keepdims=True) + epsilon)
    width = PARTS * LANES
    mine = pl.ds(pl.multiple_of(y * width, width), width)
    normed = (tokens[:, mine].astype(F32) * scale * pre[:, mine]).astype(BF16)
    stacked = jnp.concatenate([normed[:, part * LANES : (part + 1) * LANES] for part in range(PARTS)], axis=0)

    flat_sent = sent.reshape(PEERS * BLOCK, LANES)
    flat_arrived = arrived.reshape(PEERS * BLOCK, LANES)
    flat_results = results.reshape(PEERS * BLOCK, LANES)
    flat_returned = returned.reshape(PEERS * BLOCK, LANES)
    own = STEPS.index(0) * NQ * CAP
    own_chunk = max(j for j in range(CHUNKS) if EDGES[j] <= STEPS.index(0))

    def send_blocks(source, target, sends, receives, j, place):
        for q, n in ((q, n) for q in FARTHEST for n in range(EDGES[j], EDGES[j + 1])):
            if not (STEPS[n] or q):
                continue
            rows_at = pl.ds((n * NQ + q) * CAP, CAP)
            pltpu.make_async_remote_copy(
                source.at[rows_at], target.at[rows_at], sends.at[j], receives.at[j],
                device_id=place(n, q), device_id_type=MESH,
            ).start()
        if j == own_chunk:
            target[own : own + CAP] = source[own : own + CAP]

    def wait_blocks(buffer, sem, j):
        part = buffer.at[pl.ds(0, ROWS[j] - CAP if j == own_chunk else ROWS[j])]
        pltpu.make_async_copy(part, part, sem.at[j]).wait()

    def send_tp(buffer, sends, receives, j):
        for other in ys:
            pltpu.make_async_remote_copy(
                buffer[j].at[y], buffer[j].at[y], sends.at[j], receives.at[j],
                device_id={"tp": other}, device_id_type=MESH,
            ).start()

    def wait_tp(buffer, sem, j):
        part = buffer[j].at[pl.ds(0, NY - 1)]
        pltpu.make_async_copy(part, part, sem.at[j]).wait()

    def assemble(j):
        r = iota((TALL[j], rows * PARTS), 0) + BASE[j]
        take = jnp.where((r == across[0]) | (r == across[1]), 1.0, 0.0).astype(BF16)
        flat_sent[BASE[j] : BASE[j + 1], :] = dot(take, stacked).astype(BF16)

    def send(j):
        send_blocks(sent, arrived, out_sem, in_sem, j, ahead)

    order = {}
    for tall, count in dict(zip(TALL, ROWS)).items():
        shape = (tall, tall)
        order[tall] = (
            (iota(shape, 1) == tall_row(iota(shape, 0), count)).astype(BF16),
            (iota(shape, 0) == tall_row(iota(shape, 1), count)).astype(BF16),
        )

    def collect(j):
        wait_blocks(arrived, in_sem, j)
        wide = dot(order[TALL[j]][0], flat_arrived[BASE[j] : BASE[j + 1], :])
        n = ROWS[j]
        wide = jnp.concatenate([wide[part * n : (part + 1) * n] for part in range(PARTS)], axis=1)
        gathered[j][y] = wide.astype(BF16)
        send_tp(gathered, feat_out, feat_in, j)

    def gated(j):
        if j == 0:
            for load in loads[3:]:
                load.wait()
        wait_tp(gathered, feat_in, j)
        total = sum(dot(gathered[j][other], gate_up[other * width : (other + 1) * width, :]) for other in range(NY))
        gate, up = total[:, :LANES], total[:, LANES:]
        hidden[j][y] = (gate / (1.0 + jnp.exp(-gate)) * up).astype(BF16)
        send_tp(hidden, hid_out, hid_in, j)

    def project(j):
        wait_tp(hidden, hid_in, j)
        units = jnp.concatenate([hidden[j][other] for other in range(NY)], axis=1)
        made = dot(units, down[...])
        made = jnp.concatenate([made[:, part * LANES : (part + 1) * LANES] for part in range(PARTS)], axis=0)
        flat_results[BASE[j] : BASE[j + 1], :] = dot(order[TALL[j]][1], made.astype(BF16)).astype(BF16)
        send_blocks(results, returned, ret_out, ret_in, j, behind)

    def column(row):
        return jnp.transpose(jnp.broadcast_to(row, square_shape))[:, 0:1]

    columns = []

    def merge(j):
        first = not columns
        if first:
            columns.extend((column(spots[k].astype(F32)).astype(I32), column(weights[k : k + 1, :])) for k in range(2))
        r = iota((rows, TALL[j]), 1) + BASE[j]
        share = jnp.concatenate(
            [sum(jnp.where(r == s + CAP * part, w, 0.0) for s, w in columns) for part in range(PARTS)], axis=0
        )
        coarse = share.astype(BF16)
        fine = (share - coarse.astype(F32)).astype(BF16)
        wait_blocks(returned, ret_in, j)
        back = flat_returned[BASE[j] : BASE[j + 1], :]
        added = dot(coarse, back) + dot(fine, back)
        mixed[...] = added if first else mixed[...] + added

    steps = dict(A=assemble, K=hear, S=send, C=collect, G=gated, P=project, M=merge)
    for step in PLAN:
        steps[step[0]](int(step[1:]))

    pieces = [mixed[part * rows : (part + 1) * rows, :] for part in range(PARTS)]
    square = jnp.sum(sum(piece * piece for piece in pieces), axis=1, keepdims=True)
    squares[y] = jnp.transpose(jnp.broadcast_to(square, square_shape))[0:1, :]
    for other in ys:
        pltpu.make_async_remote_copy(
            squares.at[y], squares.at[y], sq_sem.at[0], sq_sem.at[1], device_id={"tp": other}, device_id_type=MESH
        ).start()
    for j in range(CHUNKS):
        wait_blocks(sent, out_sem, j)
        wait_blocks(results, ret_out, j)
        wait_tp(gathered, feat_out, j)
        wait_tp(hidden, hid_out, j)
    three = squares.at[pl.ds(0, NY - 1)]
    pltpu.make_async_copy(three, three, sq_sem.at[1]).wait()
    total = squares[0] + squares[1] + squares[2] + squares[3]
    out_scale = lax.rsqrt(total / (width * NY) + epsilon)
    out_scale = jnp.transpose(jnp.broadcast_to(out_scale, square_shape))
    for part in range(PARTS):
        o_ref[:, part * LANES : (part + 1) * LANES] = pieces[part] * out_scale
    pltpu.make_async_copy(three, three, sq_sem.at[0]).wait()


def per_device(tokens, pre_gain, post_gain, expert_ids, route_weights, w_gate, w_up, w_down):
    rows, row_width = tokens.shape
    width = PARTS * LANES
    blocks = pltpu.VMEM((PEERS * CAP, PARTS, LANES), BF16)
    sems = pltpu.SemaphoreType.DMA((CHUNKS,))
    scaled = pl.pallas_call(
        kernel,
        out_shape=pltpu.VMEM((rows, width), F32),
        in_specs=[pl.BlockSpec(memory_space=pltpu.HBM)] * 7,
        out_specs=pl.BlockSpec(memory_space=pltpu.VMEM),
        scratch_shapes=[
            pltpu.VMEM((rows, row_width), BF16),
            pltpu.VMEM((1, row_width), F32),
            pltpu.VMEM((2, rows), I32),
            pltpu.VMEM((2, rows), F32),
            pltpu.VMEM((row_width, 2 * LANES), BF16),
            pltpu.VMEM((w_down.shape[1], width), BF16),
            blocks,
            blocks,
            blocks,
            blocks,
            pltpu.VMEM((NY, 1, rows), F32),
            pltpu.VMEM((rows * PARTS, LANES), F32),
            pltpu.SemaphoreType.DMA((7,)),
            pltpu.SemaphoreType.REGULAR((3,)),
            *[sems] * 8,
            pltpu.SemaphoreType.DMA((2,)),
            *[pltpu.VMEM((NY, count, width), BF16) for count in ROWS],
            *[pltpu.VMEM((NY, count, LANES), BF16) for count in ROWS],
        ],
        compiler_params=pltpu.CompilerParams(
            collective_id=0, has_side_effects=True
        ),
    )(tokens, pre_gain[None, :], expert_ids.T, route_weights.T, w_gate, w_up, w_down)
    return (scaled * post_gain[None, :]).astype(BF16)


def solution(mesh):
    in_specs = (
        P("ep", None),
        P(),
        P("tp"),
        P("ep", None),
        P("ep", None),
        P("ep", None, "tp"),
        P("ep", None, "tp"),
        P("ep", None, "tp"),
    )
    return jax.shard_map(per_device, mesh=mesh, in_specs=in_specs, out_specs=P("ep", "tp"), check_vma=False)
```

```python
import jax
import jax.numpy as jnp
from jax import lax
from jax.experimental import pallas as pl
from jax.experimental.pallas import tpu as pltpu
from jax.sharding import PartitionSpec as P

epsilon = 1e-06
MESH = pl.DeviceIdType.MESH
NZ, NX, NC, NY = 16, 4, 2, 4
NQ = NX * NC
PEERS = NZ * NQ
FARTHEST = (5, 4, 3, 7, 2, 6, 1, 0)
CAP = 3
STEPS = (0, 1, -1, 2, -2, 3, 4, -4, -3, 8, -7, 7, -6, 6, -5, 5)
PLAN = (
    "A0", "A1", "A2", "A3", "K0", "S0", "S1", "A4", "A5", "K1", "S2", "S3", "A6", "A7", "C0", "K2", "S4", "S5",
    "S6", "S7", "C1", "C2", "C3", "G0", "G1", "G2", "G3", "P0", "P1", "C4", "P2", "C5", "P3", "G4", "C6", "G5",
    "P4", "C7", "G6", "P5", "G7", "P6", "P7", "M0", "M1", "M2", "M3", "M4", "M5", "M6", "M7",
)
NEAR = 2
EDGES = (0, 2, 4, 6, 8, 10, 12, 14, 16)
CHUNKS = len(EDGES) - 1
SPAN = [EDGES[j + 1] - EDGES[j] for j in range(CHUNKS)]
ROWS = [NQ * CAP * span for span in SPAN]
LANES = 128
PARTS = 4
BLOCK = PARTS * CAP
TALL = [NQ * BLOCK * span for span in SPAN]
BASE = [NQ * BLOCK * edge for edge in EDGES]
BF16, F32, I32 = jnp.bfloat16, jnp.float32, jnp.int32


def dot(a, b):
    return jnp.dot(a, b, preferred_element_type=F32)


def iota(shape, dim):
    return lax.broadcasted_iota(I32, shape, dim)


def tall_row(wide, rows):
    part = sum((wide >= rows * k).astype(I32) for k in range(1, PARTS))
    rest = wide - part * rows
    block = (rest * 171) >> 9
    return block * BLOCK + part * CAP + (rest - block * CAP)


def kernel(
    tokens_hbm, pre_hbm, ids_hbm, weights_hbm, gate_hbm, up_hbm, down_hbm,
    o_ref,
    tokens, pre, ids, weights, gate_up, down, sent, arrived, results, returned, squares, mixed,
    load_sem, wide_sem, out_sem, in_sem, feat_out, feat_in, hid_out, hid_in, ret_out, ret_in, sq_sem, *buffers,
):
    gathered, hidden = buffers[:CHUNKS], buffers[CHUNKS:]
    me, y = lax.axis_index("ep"), lax.axis_index("tp")
    z, x, c = lax.div(me, NQ), lax.rem(lax.div(me, NC), NX), lax.rem(me, NC)
    zs = [lax.rem(z + d, NZ) * NQ for d in range(NZ)]
    xs = [lax.rem(x + d, NX) * NC for d in range(NX)]
    cs = [c, 1 - c]
    ys = [lax.rem(y + d, NY) for d in (2, 1, 3)]

    def at(dz, q):
        return {"ep": zs[dz % NZ] + xs[q // NC] + cs[q % NC]}

    def ahead(n, q):
        return at(STEPS[n], q)

    def behind(n, q):
        return {"ep": zs[-STEPS[n] % NZ] + xs[-(q // NC) % NX] + cs[q % NC]}

    barrier = pltpu.get_barrier_semaphore()
    for other in ys:
        pl.semaphore_signal(barrier, inc=1, device_id={"tp": other}, device_id_type=MESH)
    near = range(max(-NEAR, 1 - NZ // 2), NEAR + 1)
    for dz in sorted(near, key=abs, reverse=True):
        for q in FARTHEST:
            if dz or q:
                pl.semaphore_signal(barrier, inc=1, device_id=at(dz, q), device_id_type=MESH)

    def hear(level):
        if level == 0:
            pl.semaphore_wait(barrier, len(near) * NQ - 1 + NY - 1)
        else:
            pl.semaphore_wait(wide_sem.at[level - 1], 2)
        reach = NEAR << level
        if reach < NZ // 2:
            for dz in (reach, -reach):
                pl.semaphore_signal(wide_sem.at[level], inc=1, device_id=at(dz, 0), device_id_type=MESH)

    loads = [
        pltpu.make_async_copy(ids_hbm, ids, load_sem.at[0]),
        pltpu.make_async_copy(tokens_hbm, tokens, load_sem.at[1]),
        pltpu.make_async_copy(pre_hbm, pre, load_sem.at[2]),
        pltpu.make_async_copy(weights_hbm, weights, load_sem.at[3]),
        pltpu.make_async_copy(gate_hbm.at[0], gate_up.at[:, pl.ds(0, LANES)], load_sem.at[4]),
        pltpu.make_async_copy(up_hbm.at[0], gate_up.at[:, pl.ds(LANES, LANES)], load_sem.at[5]),
        pltpu.make_async_copy(down_hbm.at[0], down, load_sem.at[6]),
    ]
    for load in loads:
        load.start()

    rows = tokens.shape[0]
    square_shape = (rows, rows)
    earlier_than = (iota(square_shape, 0) < iota(square_shape, 1)).astype(BF16)
    loads[0].wait()
    spots, before = [], None
    for k in range(2):
        e = ids[k : k + 1, :]
        dz = ((e >> 3) - z) & (NZ - 1)
        n = sum(jnp.where(dz == STEPS[i] % NZ, i, 0) for i in range(NZ))
        q = (((((e >> 1) & 3) - x) & 3) << 1) + (((e & 1) - c) & 1)
        p = n * NQ + q
        mark = (iota((PEERS, rows), 0) == p).astype(F32)
        earlier = dot(mark.astype(BF16), earlier_than)
        if before is not None:
            earlier = earlier + before
        before = jnp.sum(mark, axis=1, keepdims=True)
        slot = jnp.sum(earlier * mark, axis=0, keepdims=True)
        spots.append(p * BLOCK + slot.astype(I32))
    across = [jnp.concatenate([spot + CAP * part for part in range(PARTS)], axis=1) for spot in spots]

    loads[1].wait()
    loads[2].wait()
    values = tokens[...].astype(F32)
    scale = lax.rsqrt(jnp.mean(values * values, axis=1, keepdims=True) + epsilon)
    width = PARTS * LANES
    mine = pl.ds(pl.multiple_of(y * width, width), width)
    normed = (tokens[:, mine].astype(F32) * scale * pre[:, mine]).astype(BF16)
    stacked = jnp.concatenate([normed[:, part * LANES : (part + 1) * LANES] for part in range(PARTS)], axis=0)

    flat_sent = sent.reshape(PEERS * BLOCK, LANES)
    flat_arrived = arrived.reshape(PEERS * BLOCK, LANES)
    flat_results = results.reshape(PEERS * BLOCK, LANES)
    flat_returned = returned.reshape(PEERS * BLOCK, LANES)
    own = STEPS.index(0) * NQ * CAP
    own_chunk = max(j for j in range(CHUNKS) if EDGES[j] <= STEPS.index(0))

    def send_blocks(source, target, sends, receives, j, place):
        for q, n in ((q, n) for q in FARTHEST for n in range(EDGES[j], EDGES[j + 1])):
            if not (STEPS[n] or q):
                continue
            rows_at = pl.ds((n * NQ + q) * CAP, CAP)
            pltpu.make_async_remote_copy(
                source.at[rows_at], target.at[rows_at], sends.at[j], receives.at[j],
                device_id=place(n, q), device_id_type=MESH,
            ).start()
        if j == own_chunk:
            target[own : own + CAP] = source[own : own + CAP]

    def wait_blocks(buffer, sem, j):
        part = buffer.at[pl.ds(0, ROWS[j] - CAP if j == own_chunk else ROWS[j])]
        pltpu.make_async_copy(part, part, sem.at[j]).wait()

    def send_tp(buffer, sends, receives, j):
        for other in ys:
            pltpu.make_async_remote_copy(
                buffer[j].at[y], buffer[j].at[y], sends.at[j], receives.at[j],
                device_id={"tp": other}, device_id_type=MESH,
            ).start()

    def wait_tp(buffer, sem, j):
        part = buffer[j].at[pl.ds(0, NY - 1)]
        pltpu.make_async_copy(part, part, sem.at[j]).wait()

    def assemble(j):
        r = iota((TALL[j], rows * PARTS), 0) + BASE[j]
        take = jnp.where((r == across[0]) | (r == across[1]), 1.0, 0.0).astype(BF16)
        flat_sent[BASE[j] : BASE[j + 1], :] = dot(take, stacked).astype(BF16)

    def send(j):
        send_blocks(sent, arrived, out_sem, in_sem, j, ahead)

    order = {}
    for tall, count in dict(zip(TALL, ROWS)).items():
        shape = (tall, tall)
        order[tall] = (
            (iota(shape, 1) == tall_row(iota(shape, 0), count)).astype(BF16),
            (iota(shape, 0) == tall_row(iota(shape, 1), count)).astype(BF16),
        )

    def collect(j):
        wait_blocks(arrived, in_sem, j)
        wide = dot(order[TALL[j]][0], flat_arrived[BASE[j] : BASE[j + 1], :])
        n = ROWS[j]
        wide = jnp.concatenate([wide[part * n : (part + 1) * n] for part in range(PARTS)], axis=1)
        gathered[j][y] = wide.astype(BF16)
        send_tp(gathered, feat_out, feat_in, j)

    def gated(j):
        if j == 0:
            for load in loads[3:]:
                load.wait()
        wait_tp(gathered, feat_in, j)
        total = sum(dot(gathered[j][other], gate_up[other * width : (other + 1) * width, :]) for other in range(NY))
        gate, up = total[:, :LANES], total[:, LANES:]
        hidden[j][y] = (gate / (1.0 + jnp.exp(-gate)) * up).astype(BF16)
        send_tp(hidden, hid_out, hid_in, j)

    def project(j):
        wait_tp(hidden, hid_in, j)
        units = jnp.concatenate([hidden[j][other] for other in range(NY)], axis=1)
        made = dot(units, down[...])
        made = jnp.concatenate([made[:, part * LANES : (part + 1) * LANES] for part in range(PARTS)], axis=0)
        flat_results[BASE[j] : BASE[j + 1], :] = dot(order[TALL[j]][1], made.astype(BF16)).astype(BF16)
        send_blocks(results, returned, ret_out, ret_in, j, behind)

    def column(row):
        return jnp.transpose(jnp.broadcast_to(row, square_shape))[:, 0:1]

    columns = []

    def merge(j):
        first = not columns
        if first:
            columns.extend((column(spots[k].astype(F32)).astype(I32), column(weights[k : k + 1, :])) for k in range(2))
        r = iota((rows, TALL[j]), 1) + BASE[j]
        share = jnp.concatenate(
            [sum(jnp.where(r == s + CAP * part, w, 0.0) for s, w in columns) for part in range(PARTS)], axis=0
        )
        coarse = share.astype(BF16)
        fine = (share - coarse.astype(F32)).astype(BF16)
        wait_blocks(returned, ret_in, j)
        back = flat_returned[BASE[j] : BASE[j + 1], :]
        added = dot(coarse, back) + dot(fine, back)
        mixed[...] = added if first else mixed[...] + added

    steps = dict(A=assemble, K=hear, S=send, C=collect, G=gated, P=project, M=merge)
    for step in PLAN:
        steps[step[0]](int(step[1:]))

    pieces = [mixed[part * rows : (part + 1) * rows, :] for part in range(PARTS)]
    square = jnp.sum(sum(piece * piece for piece in pieces), axis=1, keepdims=True)
    squares[y] = jnp.transpose(jnp.broadcast_to(square, square_shape))[0:1, :]
    for other in ys:
        pltpu.make_async_remote_copy(
            squares.at[y], squares.at[y], sq_sem.at[0], sq_sem.at[1], device_id={"tp": other}, device_id_type=MESH
        ).start()
    for j in range(CHUNKS):
        wait_blocks(sent, out_sem, j)
        wait_blocks(results, ret_out, j)
        wait_tp(gathered, feat_out, j)
        wait_tp(hidden, hid_out, j)
    three = squares.at[pl.ds(0, NY - 1)]
    pltpu.make_async_copy(three, three, sq_sem.at[1]).wait()
    total = squares[0] + squares[1] + squares[2] + squares[3]
    out_scale = lax.rsqrt(total / (width * NY) + epsilon)
    out_scale = jnp.transpose(jnp.broadcast_to(out_scale, square_shape))
    for part in range(PARTS):
        o_ref[:, part * LANES : (part + 1) * LANES] = pieces[part] * out_scale
    pltpu.make_async_copy(three, three, sq_sem.at[0]).wait()


def per_device(tokens, pre_gain, post_gain, expert_ids, route_weights, w_gate, w_up, w_down):
    rows, row_width = tokens.shape
    width = PARTS * LANES
    blocks = pltpu.VMEM((PEERS * CAP, PARTS, LANES), BF16)
    sems = pltpu.SemaphoreType.DMA((CHUNKS,))
    scaled = pl.pallas_call(
        kernel,
        out_shape=pltpu.VMEM((rows, width), F32),
        in_specs=[pl.BlockSpec(memory_space=pltpu.HBM)] * 7,
        out_specs=pl.BlockSpec(memory_space=pltpu.VMEM),
        scratch_shapes=[
            pltpu.VMEM((rows, row_width), BF16),
            pltpu.VMEM((1, row_width), F32),
            pltpu.VMEM((2, rows), I32),
            pltpu.VMEM((2, rows), F32),
            pltpu.VMEM((row_width, 2 * LANES), BF16),
            pltpu.VMEM((w_down.shape[1], width), BF16),
            blocks,
            blocks,
            blocks,
            blocks,
            pltpu.VMEM((NY, 1, rows), F32),
            pltpu.VMEM((rows * PARTS, LANES), F32),
            pltpu.SemaphoreType.DMA((7,)),
            pltpu.SemaphoreType.REGULAR((3,)),
            *[sems] * 8,
            pltpu.SemaphoreType.DMA((2,)),
            *[pltpu.VMEM((NY, count, width), BF16) for count in ROWS],
            *[pltpu.VMEM((NY, count, LANES), BF16) for count in ROWS],
        ],
        compiler_params=pltpu.CompilerParams(
            collective_id=0, has_side_effects=True
        ),
    )(tokens, pre_gain[None, :], expert_ids.T, route_weights.T, w_gate, w_up, w_down)
    return (scaled * post_gain[None, :]).astype(BF16)


def solution(mesh):
    in_specs = (
        P("ep", None),
        P(),
        P("tp"),
        P("ep", None),
        P("ep", None),
        P("ep", None, "tp"),
        P("ep", None, "tp"),
        P("ep", None, "tp"),
    )
    return jax.shard_map(per_device, mesh=mesh, in_specs=in_specs, out_specs=P("ep", "tp"), check_vma=False)
```

```python
import jax
import jax.numpy as jnp
from jax import lax
from jax.experimental import pallas as pl
from jax.experimental.pallas import tpu as pltpu
from jax.sharding import PartitionSpec as P

epsilon = 1e-06
MESH = pl.DeviceIdType.MESH
NZ, NX, NC, NY = 16, 4, 2, 4
NQ = NX * NC
PEERS = NZ * NQ
FARTHEST = (5, 4, 3, 7, 2, 6, 1, 0)
CAP = 3
STEPS = (0, 1, -1, 2, -2, 3, 4, -4, -3, 8, -7, 7, -6, 6, -5, 5)
PLAN = (
    "A0", "A1", "A2", "A3", "K0", "S0", "S1", "A4", "A5", "K1", "S2", "S3", "A6", "A7", "C0", "K2", "S4", "S5",
    "S6", "S7", "C1", "C2", "C3", "G0", "G1", "G2", "G3", "P0", "P1", "C4", "P2", "C5", "P3", "G4", "C6", "G5",
    "P4", "C7", "G6", "P5", "G7", "P6", "P7", "M0", "M1", "M2", "M3", "M4", "M5", "M6", "M7",
)
NEAR = 2
EDGES = (0, 2, 4, 6, 8, 10, 12, 14, 16)
CHUNKS = len(EDGES) - 1
SPAN = [EDGES[j + 1] - EDGES[j] for j in range(CHUNKS)]
ROWS = [NQ * CAP * span for span in SPAN]
LANES = 128
PARTS = 4
BLOCK = PARTS * CAP
TALL = [NQ * BLOCK * span for span in SPAN]
BASE = [NQ * BLOCK * edge for edge in EDGES]
BF16, F32, I32 = jnp.bfloat16, jnp.float32, jnp.int32


def dot(a, b):
    return jnp.dot(a, b, preferred_element_type=F32)


def iota(shape, dim):
    return lax.broadcasted_iota(I32, shape, dim)


def tall_row(wide, rows):
    part = sum((wide >= rows * k).astype(I32) for k in range(1, PARTS))
    rest = wide - part * rows
    block = (rest * 171) >> 9
    return block * BLOCK + part * CAP + (rest - block * CAP)


def kernel(
    tokens_hbm, pre_hbm, ids_hbm, weights_hbm, gate_hbm, up_hbm, down_hbm,
    o_ref,
    tokens, pre, ids, weights, gate_up, down, sent, arrived, results, returned, squares, mixed,
    load_sem, wide_sem, out_sem, in_sem, feat_out, feat_in, hid_out, hid_in, ret_out, ret_in, sq_sem, *buffers,
):
    gathered, hidden = buffers[:CHUNKS], buffers[CHUNKS:]
    me, y = lax.axis_index("ep"), lax.axis_index("tp")
    z, x, c = lax.div(me, NQ), lax.rem(lax.div(me, NC), NX), lax.rem(me, NC)
    zs = [lax.rem(z + d, NZ) * NQ for d in range(NZ)]
    xs = [lax.rem(x + d, NX) * NC for d in range(NX)]
    cs = [c, 1 - c]
    ys = [lax.rem(y + d, NY) for d in (2, 3, 1)]

    def at(dz, q):
        return {"ep": zs[dz % NZ] + xs[q // NC] + cs[q % NC]}

    def ahead(n, q):
        return at(STEPS[n], q)

    def behind(n, q):
        return {"ep": zs[-STEPS[n] % NZ] + xs[-(q // NC) % NX] + cs[q % NC]}

    barrier = pltpu.get_barrier_semaphore()
    for other in ys:
        pl.semaphore_signal(barrier, inc=1, device_id={"tp": other}, device_id_type=MESH)
    near = range(max(-NEAR, 1 - NZ // 2), NEAR + 1)
    for dz in sorted(near, key=abs, reverse=True):
        for q in FARTHEST:
            if dz or q:
                pl.semaphore_signal(barrier, inc=1, device_id=at(dz, q), device_id_type=MESH)

    def hear(level):
        if level == 0:
            pl.semaphore_wait(barrier, len(near) * NQ - 1 + NY - 1)
        else:
            pl.semaphore_wait(wide_sem.at[level - 1], 2)
        reach = NEAR << level
        if reach < NZ // 2:
            for dz in (reach, -reach):
                pl.semaphore_signal(wide_sem.at[level], inc=1, device_id=at(dz, 0), device_id_type=MESH)

    loads = [
        pltpu.make_async_copy(ids_hbm, ids, load_sem.at[0]),
        pltpu.make_async_copy(tokens_hbm, tokens, load_sem.at[1]),
        pltpu.make_async_copy(pre_hbm, pre, load_sem.at[2]),
        pltpu.make_async_copy(weights_hbm, weights, load_sem.at[3]),
        pltpu.make_async_copy(gate_hbm.at[0], gate_up.at[:, pl.ds(0, LANES)], load_sem.at[4]),
        pltpu.make_async_copy(up_hbm.at[0], gate_up.at[:, pl.ds(LANES, LANES)], load_sem.at[5]),
        pltpu.make_async_copy(down_hbm.at[0], down, load_sem.at[6]),
    ]
    for load in loads:
        load.start()

    rows = tokens.shape[0]
    square_shape = (rows, rows)
    earlier_than = (iota(square_shape, 0) < iota(square_shape, 1)).astype(BF16)
    loads[0].wait()
    spots, before = [], None
    for k in range(2):
        e = ids[k : k + 1, :]
        dz = ((e >> 3) - z) & (NZ - 1)
        n = sum(jnp.where(dz == STEPS[i] % NZ, i, 0) for i in range(NZ))
        q = (((((e >> 1) & 3) - x) & 3) << 1) + (((e & 1) - c) & 1)
        p = n * NQ + q
        mark = (iota((PEERS, rows), 0) == p).astype(F32)
        earlier = dot(mark.astype(BF16), earlier_than)
        if before is not None:
            earlier = earlier + before
        before = jnp.sum(mark, axis=1, keepdims=True)
        slot = jnp.sum(earlier * mark, axis=0, keepdims=True)
        spots.append(p * BLOCK + slot.astype(I32))
    across = [jnp.concatenate([spot + CAP * part for part in range(PARTS)], axis=1) for spot in spots]

    loads[1].wait()
    loads[2].wait()
    values = tokens[...].astype(F32)
    scale = lax.rsqrt(jnp.mean(values * values, axis=1, keepdims=True) + epsilon)
    width = PARTS * LANES
    mine = pl.ds(pl.multiple_of(y * width, width), width)
    normed = (tokens[:, mine].astype(F32) * scale * pre[:, mine]).astype(BF16)
    stacked = jnp.concatenate([normed[:, part * LANES : (part + 1) * LANES] for part in range(PARTS)], axis=0)

    flat_sent = sent.reshape(PEERS * BLOCK, LANES)
    flat_arrived = arrived.reshape(PEERS * BLOCK, LANES)
    flat_results = results.reshape(PEERS * BLOCK, LANES)
    flat_returned = returned.reshape(PEERS * BLOCK, LANES)
    own = STEPS.index(0) * NQ * CAP
    own_chunk = max(j for j in range(CHUNKS) if EDGES[j] <= STEPS.index(0))

    def send_blocks(source, target, sends, receives, j, place):
        for q, n in ((q, n) for q in FARTHEST for n in range(EDGES[j], EDGES[j + 1])):
            if not (STEPS[n] or q):
                continue
            rows_at = pl.ds((n * NQ + q) * CAP, CAP)
            pltpu.make_async_remote_copy(
                source.at[rows_at], target.at[rows_at], sends.at[j], receives.at[j],
                device_id=place(n, q), device_id_type=MESH,
            ).start()
        if j == own_chunk:
            target[own : own + CAP] = source[own : own + CAP]

    def wait_blocks(buffer, sem, j):
        part = buffer.at[pl.ds(0, ROWS[j] - CAP if j == own_chunk else ROWS[j])]
        pltpu.make_async_copy(part, part, sem.at[j]).wait()

    def send_tp(buffer, sends, receives, j):
        for other in ys:
            pltpu.make_async_remote_copy(
                buffer[j].at[y], buffer[j].at[y], sends.at[j], receives.at[j],
                device_id={"tp": other}, device_id_type=MESH,
            ).start()

    def wait_tp(buffer, sem, j):
        part = buffer[j].at[pl.ds(0, NY - 1)]
        pltpu.make_async_copy(part, part, sem.at[j]).wait()

    def assemble(j):
        r = iota((TALL[j], rows * PARTS), 0) + BASE[j]
        take = jnp.where((r == across[0]) | (r == across[1]), 1.0, 0.0).astype(BF16)
        flat_sent[BASE[j] : BASE[j + 1], :] = dot(take, stacked).astype(BF16)

    def send(j):
        send_blocks(sent, arrived, out_sem, in_sem, j, ahead)

    order = {}
    for tall, count in dict(zip(TALL, ROWS)).items():
        shape = (tall, tall)
        order[tall] = (
            (iota(shape, 1) == tall_row(iota(shape, 0), count)).astype(BF16),
            (iota(shape, 0) == tall_row(iota(shape, 1), count)).astype(BF16),
        )

    def collect(j):
        wait_blocks(arrived, in_sem, j)
        wide = dot(order[TALL[j]][0], flat_arrived[BASE[j] : BASE[j + 1], :])
        n = ROWS[j]
        wide = jnp.concatenate([wide[part * n : (part + 1) * n] for part in range(PARTS)], axis=1)
        gathered[j][y] = wide.astype(BF16)
        send_tp(gathered, feat_out, feat_in, j)

    def gated(j):
        if j == 0:
            for load in loads[3:]:
                load.wait()
        wait_tp(gathered, feat_in, j)
        total = sum(dot(gathered[j][other], gate_up[other * width : (other + 1) * width, :]) for other in range(NY))
        gate, up = total[:, :LANES], total[:, LANES:]
        hidden[j][y] = (gate / (1.0 + jnp.exp(-gate)) * up).astype(BF16)
        send_tp(hidden, hid_out, hid_in, j)

    def project(j):
        wait_tp(hidden, hid_in, j)
        units = jnp.concatenate([hidden[j][other] for other in range(NY)], axis=1)
        made = dot(units, down[...])
        made = jnp.concatenate([made[:, part * LANES : (part + 1) * LANES] for part in range(PARTS)], axis=0)
        flat_results[BASE[j] : BASE[j + 1], :] = dot(order[TALL[j]][1], made.astype(BF16)).astype(BF16)
        send_blocks(results, returned, ret_out, ret_in, j, behind)

    def column(row):
        return jnp.transpose(jnp.broadcast_to(row, square_shape))[:, 0:1]

    columns = []

    def merge(j):
        first = not columns
        if first:
            columns.extend((column(spots[k].astype(F32)).astype(I32), column(weights[k : k + 1, :])) for k in range(2))
        r = iota((rows, TALL[j]), 1) + BASE[j]
        share = jnp.concatenate(
            [sum(jnp.where(r == s + CAP * part, w, 0.0) for s, w in columns) for part in range(PARTS)], axis=0
        )
        coarse = share.astype(BF16)
        fine = (share - coarse.astype(F32)).astype(BF16)
        wait_blocks(returned, ret_in, j)
        back = flat_returned[BASE[j] : BASE[j + 1], :]
        added = dot(coarse, back) + dot(fine, back)
        mixed[...] = added if first else mixed[...] + added

    steps = dict(A=assemble, K=hear, S=send, C=collect, G=gated, P=project, M=merge)
    for step in PLAN:
        steps[step[0]](int(step[1:]))

    pieces = [mixed[part * rows : (part + 1) * rows, :] for part in range(PARTS)]
    square = jnp.sum(sum(piece * piece for piece in pieces), axis=1, keepdims=True)
    squares[y] = jnp.transpose(jnp.broadcast_to(square, square_shape))[0:1, :]
    for other in ys:
        pltpu.make_async_remote_copy(
            squares.at[y], squares.at[y], sq_sem.at[0], sq_sem.at[1], device_id={"tp": other}, device_id_type=MESH
        ).start()
    for j in range(CHUNKS):
        wait_blocks(sent, out_sem, j)
        wait_blocks(results, ret_out, j)
        wait_tp(gathered, feat_out, j)
        wait_tp(hidden, hid_out, j)
    three = squares.at[pl.ds(0, NY - 1)]
    pltpu.make_async_copy(three, three, sq_sem.at[1]).wait()
    total = squares[0] + squares[1] + squares[2] + squares[3]
    out_scale = lax.rsqrt(total / (width * NY) + epsilon)
    out_scale = jnp.transpose(jnp.broadcast_to(out_scale, square_shape))
    for part in range(PARTS):
        o_ref[:, part * LANES : (part + 1) * LANES] = pieces[part] * out_scale
    pltpu.make_async_copy(three, three, sq_sem.at[0]).wait()


def per_device(tokens, pre_gain, post_gain, expert_ids, route_weights, w_gate, w_up, w_down):
    rows, row_width = tokens.shape
    width = PARTS * LANES
    blocks = pltpu.VMEM((PEERS * CAP, PARTS, LANES), BF16)
    sems = pltpu.SemaphoreType.DMA((CHUNKS,))
    scaled = pl.pallas_call(
        kernel,
        out_shape=pltpu.VMEM((rows, width), F32),
        in_specs=[pl.BlockSpec(memory_space=pltpu.HBM)] * 7,
        out_specs=pl.BlockSpec(memory_space=pltpu.VMEM),
        scratch_shapes=[
            pltpu.VMEM((rows, row_width), BF16),
            pltpu.VMEM((1, row_width), F32),
            pltpu.VMEM((2, rows), I32),
            pltpu.VMEM((2, rows), F32),
            pltpu.VMEM((row_width, 2 * LANES), BF16),
            pltpu.VMEM((w_down.shape[1], width), BF16),
            blocks,
            blocks,
            blocks,
            blocks,
            pltpu.VMEM((NY, 1, rows), F32),
            pltpu.VMEM((rows * PARTS, LANES), F32),
            pltpu.SemaphoreType.DMA((7,)),
            pltpu.SemaphoreType.REGULAR((3,)),
            *[sems] * 8,
            pltpu.SemaphoreType.DMA((2,)),
            *[pltpu.VMEM((NY, count, width), BF16) for count in ROWS],
            *[pltpu.VMEM((NY, count, LANES), BF16) for count in ROWS],
        ],
        compiler_params=pltpu.CompilerParams(
            collective_id=0, has_side_effects=True
        ),
    )(tokens, pre_gain[None, :], expert_ids.T, route_weights.T, w_gate, w_up, w_down)
    return (scaled * post_gain[None, :]).astype(BF16)


def solution(mesh):
    in_specs = (
        P("ep", None),
        P(),
        P("tp"),
        P("ep", None),
        P("ep", None),
        P("ep", None, "tp"),
        P("ep", None, "tp"),
        P("ep", None, "tp"),
    )
    return jax.shard_map(per_device, mesh=mesh, in_specs=in_specs, out_specs=P("ep", "tp"), check_vma=False)
```
